32 devices in a mesh: sp: 8 (over z, y), tp: 4 (over x, core).
Axes of the slice: x: 2, y: 2, z: 4, core: 2. Of those that a mesh axis runs over, the one named last changes fastest.
Arguments:
- tokens: bfloat16 [2048, 2048], P('sp'), may hold values from -72 to 72
- query_weight: bfloat16 [3, 2048, 1024], P(None, None, 'tp'), may hold values from -0.125 to 0.125
- key_weight: bfloat16 [3, 2048, 1024], P(None, None, 'tp'), may hold values from -0.125 to 0.125
- value_weight: bfloat16 [3, 2048, 1024], P(None, None, 'tp'), may hold values from -0.125 to 0.125
- out_weight: bfloat16 [1024, 2048], P(None, 'tp'), may hold values from -2 to 2
Outputs:
- mixed: bfloat16 [2048, 2048], P('sp', 'tp')
The draws below stay inside these ranges and needn't reach their ends.
All inputs are finite; a program needn't handle non-finite values.
Results may differ from the reference program's by a relative error of at most 0.012.
Values may be sent and summed in bfloat16 or wider, within the bound.
A program may use at most 64 MiB of HBM per device.

```python
import math
import jax
import jax.numpy as jnp
from jax import lax

D = 2048
SLOTS = 16
HEAD_DIM = 64
SIDE_STEPS = 64
MIDDLE_DILATION = 4
FAR_DILATION = 16
HW = 1024
TOKENS = 2048


def draw_tokens(key, part):
    base = jnp.clip(jax.random.normal(key, (TOKENS, D), jnp.float32), -6.0, 6.0)
    return base.astype(jnp.bfloat16)


def shard_levels(stream_key, extent, cuts, low, high):
    def one(position, blocks):
        draws = jax.random.uniform(jax.random.fold_in(jax.random.fold_in(stream_key, 6), position), (blocks,), jnp.float32, low / len(cuts), high / len(cuts))
        return jnp.repeat(jnp.exp(draws), extent[position] // blocks).reshape((-1,) + (1,) * (len(extent) - position - 1))

    level = one(*cuts[0])
    for cut in cuts[1:]:
        level = level * one(*cut)
    return level


def centred(rng, shape, spread, limit, pieces=(), kind=jnp.bfloat16):
    values = jax.random.normal(rng, shape, jnp.float32) * spread
    if len(pieces) > 0:
        values = shard_levels(rng, shape, pieces, -0.22, 0.18) * values
    return jnp.clip(values, min=-limit, max=limit).astype(kind)


def setup_inputs(seed: int = 0) -> dict:
    seeds = jax.random.split(jax.random.key(seed), 6)
    return {
        "tokens": draw_tokens(jax.random.fold_in(seeds[5], 71), 0),
        "query_weight": centred(seeds[1], (3, D, HW), D ** -0.5, 0.125, ((2, 4),)),
        "key_weight": centred(seeds[2], (3, D, HW), D ** -0.5, 0.125, ((2, 4),)),
        "value_weight": centred(seeds[3], (3, D, HW), D ** -0.5, 0.125, ((2, 4),)),
        "out_weight": centred(seeds[4], (HW, D), (HW // 128) ** -0.5, 2.0, ((1, 4),)),
    }


def rotate(projected, offset_pos):
    length, columns = projected.shape
    heads = columns // HEAD_DIM
    half = HEAD_DIM // 2
    positions = (offset_pos + jnp.arange(length)).astype(jnp.float32)
    inverse = 1.0 / (10000.0 ** (jnp.arange(half, dtype=jnp.float32) * 2.0 / HEAD_DIM))
    angles = positions[:, None] * inverse[None, :]
    angles = jnp.concatenate([angles, angles], axis=-1)
    cosine_table = jnp.cos(angles)[:, None, :]
    sine = jnp.sin(angles)[:, None, :]
    shaped = projected.reshape(length, heads, HEAD_DIM)
    turned = jnp.concatenate([-shaped[..., half:], shaped[..., :half]], axis=-1)
    return (shaped * cosine_table + turned * sine).reshape(length, columns)


def banded(queries, key_ext, value_ext, dilation, offset_pos, seq_len):
    length, columns = queries.shape
    heads = columns // HEAD_DIM
    class_len = length // dilation
    block_len = math.gcd(SIDE_STEPS, class_len)
    blocks = class_len // block_len
    extra = 2 * SIDE_STEPS // block_len
    query_blocks = queries.reshape(blocks, block_len, dilation, heads, HEAD_DIM)
    key_blocks = key_ext.reshape(blocks + extra, block_len, dilation, heads, HEAD_DIM)
    value_blocks = value_ext.reshape(blocks + extra, block_len, dilation, heads, HEAD_DIM)
    key_win = jnp.concatenate([key_blocks[shift_idx:shift_idx + blocks] for shift_idx in range(extra + 1)], axis=1)
    value_win = jnp.concatenate([value_blocks[shift_idx:shift_idx + blocks] for shift_idx in range(extra + 1)], axis=1)
    scores = jnp.einsum('bqrhe,bkrhe->brhqk', query_blocks.astype(jnp.float32), key_win.astype(jnp.float32))
    scores = scores * (HEAD_DIM ** -0.5)
    width_keys = key_win.shape[1]
    relative = jnp.arange(width_keys)[None, :] - jnp.arange(block_len)[:, None]
    within = (relative >= 0) & (relative <= 2 * SIDE_STEPS)
    key_rows = jnp.arange(blocks)[:, None] * block_len + jnp.arange(width_keys)[None, :]
    spots = offset_pos - SIDE_STEPS * dilation + dilation * key_rows[:, :, None] + jnp.arange(dilation)[None, None, :]
    inside = (spots >= 0) & (spots < seq_len)
    allowed = within[None, None, None] & jnp.transpose(inside, (0, 2, 1))[:, :, None, None, :]
    scores = jnp.where(allowed, scores, -1e30)
    row_max = jnp.max(scores, axis=-1, keepdims=True)
    expo = jnp.exp(scores - row_max)
    denom = jnp.sum(expo, axis=-1)
    probs = lax.optimization_barrier(expo.astype(jnp.bfloat16))
    summed = jnp.einsum('brhqk,bkrhe->bqrhe', probs.astype(jnp.float32), value_win.astype(jnp.float32))
    group_out = summed / jnp.transpose(denom, (0, 3, 1, 2))[..., None]
    log_sum = row_max[..., 0] + jnp.log(denom)
    log_sum = jnp.transpose(log_sum, (0, 3, 1, 2)).reshape(length, heads)
    return group_out.reshape(length, columns), log_sum


def reference(tokens, query_weight, key_weight, value_weight, out_weight):
    seq_len = tokens.shape[0]
    group_dilations = (1, MIDDLE_DILATION, FAR_DILATION)
    outputs = []
    log_sums = []
    for group_idx in range(3):
        queries = rotate(jnp.dot(tokens, query_weight[group_idx], preferred_element_type=jnp.float32), 0).astype(jnp.bfloat16)
        keys_all = rotate(jnp.dot(tokens, key_weight[group_idx], preferred_element_type=jnp.float32), 0).astype(jnp.bfloat16)
        value_rows_full = jnp.dot(tokens, value_weight[group_idx], preferred_element_type=jnp.float32).astype(jnp.bfloat16)
        reach = SIDE_STEPS * group_dilations[group_idx]
        key_ext = jnp.pad(keys_all, ((reach, reach), (0, 0)))
        value_ext = jnp.pad(value_rows_full, ((reach, reach), (0, 0)))
        group_out, log_sum = banded(queries, key_ext, value_ext, group_dilations[group_idx], 0, seq_len)
        outputs.append(group_out)
        log_sums.append(log_sum)
    merge_w = jax.nn.softmax(jnp.stack(log_sums, axis=0), axis=0)
    stacked = jnp.stack(outputs, axis=0).reshape(3, seq_len, SLOTS, HEAD_DIM)
    merged = jnp.sum(merge_w[..., None] * stacked, axis=0).reshape(seq_len, HW).astype(jnp.bfloat16)
    return jnp.dot(merged, out_weight, preferred_element_type=jnp.float32).astype(jnp.bfloat16)
```

```python
import functools
import math

import jax
import numpy as np
import jax.numpy as jnp
from jax import lax
from jax.experimental import pallas as pl
from jax.experimental.pallas import tpu as pltpu
from jax.sharding import PartitionSpec as P

HEAD_DIM = 64
SIDE_STEPS = 64
MIDDLE_DILATION = 4
FAR_DILATION = 16
MESH = pl.DeviceIdType.MESH


def shifted(block, axis, distance):
    devices = range(lax.axis_size(axis))
    route = [(i - distance, i) for i in devices if i - distance in devices]
    return lax.ppermute(block, axis, route)


def with_halo(block, sides, width):
    for axis, dim in sides:
        count = lax.axis_size(axis)
        forward = [(i, i + 1) for i in range(count - 1)]
        backward = [(target, source) for source, target in forward]
        low = lax.ppermute(
            lax.slice_in_dim(block, block.shape[dim] - width, None, axis=dim), axis, forward
        )
        high = lax.ppermute(lax.slice_in_dim(block, 0, width, axis=dim), axis, backward)
        block = jnp.concatenate([low, block, high], axis=dim)
    return block


def rotate(projected, offset_pos):
    length, columns = projected.shape
    heads = columns // HEAD_DIM
    half = HEAD_DIM // 2
    positions = (offset_pos + jnp.arange(length)).astype(jnp.float32)
    inverse = 1.0 / 10000.0 ** (jnp.arange(half, dtype=jnp.float32) * 2.0 / HEAD_DIM)
    angles = positions[:, None] * inverse[None, :]
    angles = jnp.concatenate([angles, angles], axis=-1)
    cosine_table = jnp.cos(angles)[:, None, :]
    sine = jnp.sin(angles)[:, None, :]
    shaped = projected.reshape(length, heads, HEAD_DIM)
    turned = jnp.concatenate([-shaped[..., half:], shaped[..., :half]], axis=-1)
    return (shaped * cosine_table + turned * sine).reshape(length, columns)


def banded(queries, key_ext, value_ext, dilation, offset_pos, seq_len):
    length, columns = queries.shape
    heads = columns // HEAD_DIM
    class_len = length // dilation
    block_len = math.gcd(SIDE_STEPS, class_len)
    blocks = class_len // block_len
    extra = 2 * SIDE_STEPS // block_len
    query_blocks = queries.reshape(blocks, block_len, dilation, heads, HEAD_DIM)
    key_blocks = key_ext.reshape(blocks + extra, block_len, dilation, heads, HEAD_DIM)
    value_blocks = value_ext.reshape(blocks + extra, block_len, dilation, heads, HEAD_DIM)
    key_win = jnp.concatenate(
        [key_blocks[shift_idx : shift_idx + blocks] for shift_idx in range(extra + 1)], axis=1
    )
    value_win = jnp.concatenate(
        [value_blocks[shift_idx : shift_idx + blocks] for shift_idx in range(extra + 1)], axis=1
    )
    scores = jnp.einsum(
        "bqrhe,bkrhe->brhqk", query_blocks, key_win, preferred_element_type=jnp.float32
    )
    scores = scores * HEAD_DIM ** (-0.5)
    width_keys = key_win.shape[1]
    relative = jnp.arange(width_keys)[None, :] - jnp.arange(block_len)[:, None]
    within = (relative >= 0) & (relative <= 2 * SIDE_STEPS)
    key_rows = jnp.arange(blocks)[:, None] * block_len + jnp.arange(width_keys)[None, :]
    spots = (
        offset_pos
        - SIDE_STEPS * dilation
        + dilation * key_rows[:, :, None]
        + jnp.arange(dilation)[None, None, :]
    )
    inside = (spots >= 0) & (spots < seq_len)
    allowed = within[None, None, None] & jnp.transpose(inside, (0, 2, 1))[:, :, None, None, :]
    scores = jnp.where(allowed, scores, -1e30)
    row_max = jnp.max(scores, axis=-1, keepdims=True)
    expo = jnp.exp(scores - row_max)
    denom = jnp.sum(expo, axis=-1)
    probs = expo.astype(jnp.bfloat16)
    summed = jnp.einsum("brhqk,bkrhe->bqrhe", probs, value_win, preferred_element_type=jnp.float32)
    group_out = summed / jnp.transpose(denom, (0, 3, 1, 2))[..., None]
    log_sum = row_max[..., 0] + jnp.log(denom)
    log_sum = jnp.transpose(log_sum, (0, 3, 1, 2)).reshape(length, heads)
    return (group_out.reshape(length, columns), log_sum)


def collect(own_block, needed, direction):
    collected = own_block[None]
    while collected.shape[0] < needed + 1:
        stride = collected.shape[0]
        to_send = min(stride, needed + 1 - stride)
        arrived = shifted(collected[:to_send], "sp", direction * stride)
        collected = jnp.concatenate([collected, arrived], axis=0)
    return collected[1:]


def per_device(tokens, query_weight, key_weight, value_weight, out_weight):
    length = tokens.shape[0]
    offset_pos = lax.axis_index("sp") * length
    seq_len = lax.axis_size("sp") * length
    group_dilations = (1, MIDDLE_DILATION, FAR_DILATION)
    query_list = []
    pairs = []
    for group_idx in range(3):
        queries = rotate(
            jnp.dot(tokens, query_weight[group_idx], preferred_element_type=jnp.float32), offset_pos
        )
        keys_here = rotate(
            jnp.dot(tokens, key_weight[group_idx], preferred_element_type=jnp.float32), offset_pos
        )
        values_here = jnp.dot(tokens, value_weight[group_idx], preferred_element_type=jnp.float32)
        query_list.append(queries.astype(jnp.bfloat16))
        pairs.append(
            jnp.stack([keys_here.astype(jnp.bfloat16), values_here.astype(jnp.bfloat16)], axis=0)
        )
    middle_span_length = SIDE_STEPS * MIDDLE_DILATION
    first_ext = with_halo(pairs[0], (("sp", 1),), SIDE_STEPS)
    middle_ext = with_halo(pairs[1], (("sp", 1),), middle_span_length)
    far_span_length = SIDE_STEPS * FAR_DILATION
    needed = -(-far_span_length // length)
    lower_blocks = collect(pairs[2], needed, 1)
    upper_blocks = collect(pairs[2], needed, -1)
    columns = pairs[2].shape[2]
    lower_flat = jnp.moveaxis(lower_blocks[::-1], 0, 1).reshape(2, needed * length, columns)
    upper_flat = jnp.moveaxis(upper_blocks, 0, 1).reshape(2, needed * length, columns)
    far_full = jnp.concatenate([lower_flat, pairs[2], upper_flat], axis=1)
    extended = (first_ext, middle_ext, far_full)
    outputs = []
    log_sums = []
    for group_idx in range(3):
        group_out, log_sum = banded(
            query_list[group_idx],
            extended[group_idx][0],
            extended[group_idx][1],
            group_dilations[group_idx],
            offset_pos,
            seq_len,
        )
        outputs.append(group_out)
        log_sums.append(log_sum)
    merge_w = jax.nn.softmax(jnp.stack(log_sums, axis=0), axis=0)
    heads = columns // HEAD_DIM
    stacked = jnp.stack(outputs, axis=0).reshape(3, length, heads, HEAD_DIM)
    merged = (
        jnp.sum(merge_w[..., None] * stacked, axis=0).reshape(length, columns).astype(jnp.bfloat16)
    )
    mixed = jnp.dot(
        lax.all_gather(merged, "tp", axis=1, tiled=True),
        out_weight,
        preferred_element_type=jnp.float32,
    )
    return mixed.astype(jnp.bfloat16)


def remote(src, dst, send_sem, recv_sem, axis, target):
    return pltpu.make_async_remote_copy(
        src_ref=src,
        dst_ref=dst,
        send_sem=send_sem,
        recv_sem=recv_sem,
        device_id={axis: target},
        device_id_type=MESH,
    )


def head_mask(columns, head):
    lane = lax.broadcasted_iota(jnp.int32, (1, columns), 1)
    return (lane // HEAD_DIM == head).astype(jnp.float32)


def attend(queries, keys, values, bias):
    rows, columns = queries.shape
    heads = columns // HEAD_DIM
    masks = [head_mask(columns, head) for head in range(heads)]
    stacked = jnp.concatenate([queries * mask.astype(jnp.bfloat16) for mask in masks], axis=0)
    scores = lax.dot_general(
        stacked, keys, (((1,), (1,)), ((), ())), preferred_element_type=jnp.float32
    )
    width = keys.shape[0]
    scores = (scores.reshape(heads, rows, width) + bias[None]).reshape(heads * rows, width)
    row_max = jnp.max(scores, axis=-1, keepdims=True)
    expo = jnp.exp(scores - row_max)
    denom = jnp.sum(expo, axis=-1, keepdims=True)
    summed = jnp.dot(expo.astype(jnp.bfloat16), values, preferred_element_type=jnp.float32)
    summed = summed / denom
    lse = row_max + jnp.log(denom)
    parts = [slice(head * rows, (head + 1) * rows) for head in range(heads)]
    out = sum(summed[part] * mask for part, mask in zip(parts, masks))
    return out, [lse[part] for part in parts]


def packed_lse(lses):
    heads = len(lses)
    lane = lax.broadcasted_iota(jnp.int32, (1, 128), 1)
    spread = sum(lse * (lane % heads == head).astype(jnp.float32) for head, lse in enumerate(lses))
    total = jnp.zeros_like(spread)
    for term in range(3):
        rounded = spread.astype(jnp.bfloat16).astype(jnp.float32)
        total = total + rounded * (lane // heads == term).astype(jnp.float32)
        spread = spread - rounded
    return total.astype(jnp.bfloat16)


def band_bias(rows, width, offset, low, high):
    query = lax.broadcasted_iota(jnp.int32, (rows, width), 0)
    key = lax.broadcasted_iota(jnp.int32, (rows, width), 1)
    step = key + offset - query
    keep = (step >= -SIDE_STEPS) & (step <= SIDE_STEPS) & (key >= low) & (key < high)
    return jnp.where(keep, 0.0, -1e30)


def permutation(length, dilation, inverse):
    row = lax.broadcasted_iota(jnp.int32, (length, length), 1 if inverse else 0)
    column = lax.broadcasted_iota(jnp.int32, (length, length), 0 if inverse else 1)
    steps = length // dilation
    source = (row % steps) * dilation + row // steps
    return (source == column).astype(jnp.float32).astype(jnp.bfloat16)


def fused_kernel(
    n, m, tokens_hbm, query_hbm, key_hbm, value_hbm, out_hbm, table_hbm, base_ref, result_ref,
    tokens, weights, out_weight, table, kv_first, kv_middle, far_send, far_recv,
    back_send, back_recv, merged_all, load_sem, weight_sem, local_sem,
    near_send_sem, near_recv_sem, far_send_sem, far_recv_sem, back_send_sem, back_recv_sem,
    tp_send_sem, tp_recv_sem,
):
    me = lax.axis_index("sp")
    mine = lax.axis_index("tp")
    length, columns = tokens.shape[0], weights.shape[-1]
    half = HEAD_DIM // 2
    classes = FAR_DILATION // n
    halo = SIDE_STEPS

    loads = [
        pltpu.make_async_copy(tokens_hbm, tokens, load_sem.at[0]),
        pltpu.make_async_copy(table_hbm, table, load_sem.at[1]),
        pltpu.make_async_copy(out_hbm, out_weight, load_sem.at[2]),
    ]
    weight_loads = {}
    loads[0].start()
    for group in (2, 1, 0):
        for kind, source in ((1, key_hbm), (2, value_hbm), (0, query_hbm)):
            slot = group * 3 + kind
            weight_loads[group, kind] = pltpu.make_async_copy(
                source.at[group], weights.at[slot], weight_sem.at[slot]
            )
            weight_loads[group, kind].start()
            if group == 2 and kind == 1:
                loads[1].start()
    loads[2].start()

    barrier = pltpu.get_barrier_semaphore()
    for distance in range(1, n):
        pl.semaphore_signal(
            barrier, inc=1, device_id={"sp": lax.rem(me + distance, n)}, device_id_type=MESH
        )
    for distance in range(1, m):
        pl.semaphore_signal(
            barrier, inc=1, device_id={"tp": lax.rem(mine + distance, m)}, device_id_type=MESH
        )

    @pl.when(me == 0)
    def _():
        kv_first[:, :halo] = jnp.zeros((2, halo, columns), jnp.bfloat16)
        kv_middle[:, :, 0] = jnp.zeros_like(kv_middle[:, :, 0])

    @pl.when(me == n - 1)
    def _():
        kv_first[:, halo + length :] = jnp.zeros((2, halo, columns), jnp.bfloat16)
        kv_middle[:, :, 2] = jnp.zeros_like(kv_middle[:, :, 2])

    loads[1].wait()
    base_cos = base_ref[0, pl.ds(me, 1), :]
    base_sin = base_ref[1, pl.ds(me, 1), :]
    cosine = base_cos * table[0] - base_sin * table[1]
    sine = base_sin * table[0] + base_cos * table[1]
    wide = columns // cosine.shape[1]
    lane = lax.broadcasted_iota(jnp.int32, (1, columns), 1)
    first_half = lane % HEAD_DIM < half
    cosine = jnp.concatenate([cosine] * wide, axis=1)
    sine = jnp.concatenate([sine] * wide, axis=1) * jnp.where(first_half, -1.0, 1.0)
    far_order = permutation(length, FAR_DILATION, False)
    middle_order = permutation(length, MIDDLE_DILATION, False)
    loads[0].wait()

    def project(group, kind):
        weight_loads[group, kind].wait()
        product = jnp.dot(
            tokens[...], weights[group * 3 + kind], preferred_element_type=jnp.float32
        )
        if kind < 2:
            later = pltpu.roll(product, columns - half, 1)
            earlier = pltpu.roll(product, half, 1)
            product = product * cosine + jnp.where(first_half, later, earlier) * sine
        if kind == 0:
            product = product * HEAD_DIM ** (-0.5)
        return product.astype(jnp.bfloat16)

    def ordered(order, block):
        return jnp.dot(order, block, preferred_element_type=jnp.float32).astype(jnp.bfloat16)

    for kind in (1, 2, 0):
        far_send[kind] = ordered(far_order, project(2, kind)).reshape(far_send.shape[1:])
    pl.semaphore_wait(barrier, n - 1 + m - 1)
    far_copies = []
    for distance in range(1, n):
        target = lax.rem(me + distance, n)
        copy = remote(
            far_send.at[:, pl.ds(target * classes, classes)],
            far_recv.at[:, :, me],
            far_send_sem.at[distance],
            far_recv_sem.at[distance],
            "sp",
            target,
        )
        copy.start()
        far_copies.append(copy)
    far_own = pltpu.make_async_copy(
        far_send.at[:, pl.ds(me * classes, classes)], far_recv.at[:, :, me], local_sem.at[0]
    )
    far_own.start()

    for kind in (1, 2):
        kv_middle[kind - 1, :, 1] = ordered(middle_order, project(1, kind)).reshape(
            MIDDLE_DILATION, length // MIDDLE_DILATION, columns
        )
    middle_up = remote(
        kv_middle.at[:, :, 1], kv_middle.at[:, :, 0],
        near_send_sem.at[0], near_recv_sem.at[0], "sp", lax.rem(me + 1, n),
    )
    middle_down = remote(
        kv_middle.at[:, :, 1], kv_middle.at[:, :, 2],
        near_send_sem.at[1], near_recv_sem.at[1], "sp", lax.rem(me + n - 1, n),
    )
    first_up = remote(
        kv_first.at[:, pl.ds(length, halo)], kv_first.at[:, pl.ds(0, halo)],
        near_send_sem.at[2], near_recv_sem.at[2], "sp", lax.rem(me + 1, n),
    )
    first_down = remote(
        kv_first.at[:, pl.ds(halo, halo)], kv_first.at[:, pl.ds(halo + length, halo)],
        near_send_sem.at[3], near_recv_sem.at[3], "sp", lax.rem(me + n - 1, n),
    )

    @pl.when(me < n - 1)
    def _():
        middle_up.start()

    @pl.when(me > 0)
    def _():
        middle_down.start()

    for kind in (1, 2):
        kv_first[kind - 1, halo : halo + length] = project(0, kind)

    @pl.when(me < n - 1)
    def _():
        first_up.start()

    @pl.when(me > 0)
    def _():
        first_down.start()

    middle_queries = ordered(middle_order, project(1, 0))
    first_queries = project(0, 0)

    far_own.wait()
    for copy in far_copies:
        copy.wait()
    class_len = n * (length // FAR_DILATION)
    far_bias = band_bias(class_len, class_len, 0, 0, class_len)
    for index in range(classes):
        queries, keys, values = (
            far_recv[kind, index].reshape(class_len, columns) for kind in range(3)
        )
        out, lses = attend(queries, keys, values, far_bias)
        back_send[index, :, :, :columns] = out.astype(jnp.bfloat16).reshape(n, -1, columns)
        back_send[index, :, :, columns:] = packed_lse(lses).reshape(n, -1, 128)
    back_copies = []
    for distance in range(1, n):
        target = lax.rem(me + distance, n)
        copy = remote(
            back_send.at[:, target],
            back_recv.at[pl.ds(me * classes, classes)],
            back_send_sem.at[distance],
            back_recv_sem.at[distance],
            "sp",
            target,
        )
        copy.start()
        back_copies.append(copy)
    back_own = pltpu.make_async_copy(
        back_send.at[:, me], back_recv.at[pl.ds(me * classes, classes)], local_sem.at[1]
    )
    back_own.start()

    @pl.when(me < n - 1)
    def _():
        first_up.wait_send()
        first_down.wait_recv()

    @pl.when(me > 0)
    def _():
        first_down.wait_send()
        first_up.wait_recv()

    tile = 2 * halo
    first_outs = []
    first_lses = []
    for start in range(0, length, tile):
        width = tile + 2 * halo
        low = halo - start - me * length
        high = halo - start + (n - me) * length
        out, lses = attend(
            first_queries[start : start + tile],
            kv_first[0, start : start + width],
            kv_first[1, start : start + width],
            band_bias(tile, width, -halo, low, high),
        )
        first_outs.append(out)
        first_lses.append(
            sum(lse * head_mask(columns, head) for head, lse in enumerate(lses))
        )
    first_out = jnp.concatenate(first_outs, axis=0)
    first_lse = jnp.concatenate(first_lses, axis=0)

    @pl.when(me < n - 1)
    def _():
        middle_up.wait_send()
        middle_down.wait_recv()

    @pl.when(me > 0)
    def _():
        middle_down.wait_send()
        middle_up.wait_recv()

    steps = length // MIDDLE_DILATION
    low = jnp.where(me == 0, steps, 0)
    high = jnp.where(me == n - 1, 2 * steps, 3 * steps)
    middle_bias = band_bias(steps, 3 * steps, -steps, low, high)
    middle_parts = []
    for index in range(MIDDLE_DILATION):
        out, lses = attend(
            middle_queries[index * steps : (index + 1) * steps],
            kv_middle[0, index].reshape(3 * steps, columns),
            kv_middle[1, index].reshape(3 * steps, columns),
            middle_bias,
        )
        middle_parts.append(
            jnp.concatenate([out.astype(jnp.bfloat16), packed_lse(lses)], axis=1)
        )

    heads = columns // HEAD_DIM
    term = lax.broadcasted_iota(jnp.int32, (128, columns), 0)
    column = lax.broadcasted_iota(jnp.int32, (128, columns), 1)
    spread = (term % heads == column // HEAD_DIM) & (term < 3 * heads)
    spread = spread.astype(jnp.float32).astype(jnp.bfloat16)

    def natural(dilation, block):
        block = jnp.dot(
            permutation(length, dilation, True), block, preferred_element_type=jnp.float32
        )
        lse = jnp.dot(
            block[:, columns:].astype(jnp.bfloat16), spread, preferred_element_type=jnp.float32
        )
        return block[:, :columns], lse

    middle_out, middle_lse = natural(MIDDLE_DILATION, jnp.concatenate(middle_parts, axis=0))

    back_own.wait()
    for copy in back_copies:
        copy.wait()
    far_out, far_lse = natural(
        FAR_DILATION, back_recv[...].reshape(length, back_recv.shape[2])
    )

    top = jnp.maximum(jnp.maximum(first_lse, middle_lse), far_lse)
    first_w = jnp.exp(first_lse - top)
    middle_w = jnp.exp(middle_lse - top)
    far_w = jnp.exp(far_lse - top)
    merged = (first_w * first_out + middle_w * middle_out + far_w * far_out) / (
        first_w + middle_w + far_w
    )
    merged_all[0] = merged.astype(jnp.bfloat16)

    tp_copies = []
    for distance in range(1, m):
        copy = remote(
            merged_all.at[0],
            merged_all.at[distance],
            tp_send_sem.at[distance],
            tp_recv_sem.at[distance],
            "tp",
            lax.rem(mine + distance, m),
        )
        copy.start()
        tp_copies.append(copy)
    loads[2].wait()
    total = jnp.zeros(result_ref.shape, jnp.float32)
    for distance in range(m):
        if distance > 0:
            tp_copies[distance - 1].wait()
        owner = lax.rem(mine - distance + m, m)
        rows = pl.ds(pl.multiple_of(owner * columns, columns), columns)
        total = total + jnp.dot(
            merged_all[distance], out_weight[rows, :], preferred_element_type=jnp.float32
        )
    result_ref[...] = total.astype(jnp.bfloat16)


def turn_tables(n, length):
    half = HEAD_DIM // 2
    inverse = 1.0 / 10000.0 ** (np.arange(half, dtype=np.float32) * np.float32(2.0) / HEAD_DIM)
    inverse = np.tile(inverse.astype(np.float64), 128 // half)[None]
    inner = np.arange(length)[:, None] * inverse
    outer = (np.arange(n) * length)[:, None] * inverse
    table = np.stack([np.cos(inner), np.sin(inner)]).astype(np.float32)
    base = np.stack([np.cos(outer), np.sin(outer)]).astype(np.float32)
    return table, base


def fused(n, m, tokens, query_weight, key_weight, value_weight, out_weight):
    length, width = tokens.shape
    columns = query_weight.shape[2]
    table, base = turn_tables(n, length)
    steps = length // FAR_DILATION
    classes = FAR_DILATION // n
    kept = columns + 128
    bf16 = jnp.bfloat16
    hbm = pl.BlockSpec(memory_space=pl.ANY)
    vmem = pl.BlockSpec(memory_space=pltpu.VMEM)
    dma = pltpu.SemaphoreType.DMA
    return pl.pallas_call(
        functools.partial(fused_kernel, n, m),
        out_shape=jax.ShapeDtypeStruct((length, out_weight.shape[1]), bf16),
        in_specs=[hbm] * 6 + [vmem],
        out_specs=vmem,
        scratch_shapes=[
            pltpu.VMEM((length, width), bf16),
            pltpu.VMEM((9, width, columns), bf16),
            pltpu.VMEM(out_weight.shape, bf16),
            pltpu.VMEM(table.shape, jnp.float32),
            pltpu.VMEM((2, length + 2 * SIDE_STEPS, columns), bf16),
            pltpu.VMEM((2, MIDDLE_DILATION, 3, length // MIDDLE_DILATION, columns), bf16),
            pltpu.VMEM((3, FAR_DILATION, steps, columns), bf16),
            pltpu.VMEM((3, classes, n, steps, columns), bf16),
            pltpu.VMEM((classes, n, steps, kept), bf16),
            pltpu.VMEM((FAR_DILATION, steps, kept), bf16),
            pltpu.VMEM((m, length, columns), bf16),
            dma((3,)),
            dma((9,)),
            dma((2,)),
            dma((4,)),
            dma((4,)),
            dma((n,)),
            dma((n,)),
            dma((n,)),
            dma((n,)),
            dma((m,)),
            dma((m,)),
        ],
        compiler_params=pltpu.CompilerParams(
            collective_id=0, has_side_effects=True, vmem_limit_bytes=60 * 1024 * 1024
        ),
    )(tokens, query_weight, key_weight, value_weight, out_weight, jnp.asarray(table), jnp.asarray(base))


def planned(n, m, *arrays):
    length, columns = arrays[0].shape[0], arrays[1].shape[2]
    fits = (
        n > 1
        and m > 1
        and FAR_DILATION % n == 0
        and length == SIDE_STEPS * MIDDLE_DILATION
        and length % (FAR_DILATION * 16) == 0
        and columns % 128 == 0
        and 3 * (columns // HEAD_DIM) <= 128
    )
    if fits:
        return fused(n, m, *arrays)
    return per_device(*arrays)


def solution(mesh):
    placed = (
        P("sp", None),
        P(None, None, "tp"),
        P(None, None, "tp"),
        P(None, None, "tp"),
        P(None, "tp"),
    )
    return jax.shard_map(
        functools.partial(planned, mesh.shape["sp"], mesh.shape["tp"]),
        mesh=mesh,
        in_specs=placed,
        out_specs=P("sp", "tp"),
        check_vma=False,
    )
```

```python
import functools
import math

import jax
import numpy as np
import jax.numpy as jnp
from jax import lax
from jax.experimental import pallas as pl
from jax.experimental.pallas import tpu as pltpu
from jax.sharding import PartitionSpec as P

HEAD_DIM = 64
SIDE_STEPS = 64
MIDDLE_DILATION = 4
FAR_DILATION = 16
MESH = pl.DeviceIdType.MESH


def shifted(block, axis, distance):
    devices = range(lax.axis_size(axis))
    route = [(i - distance, i) for i in devices if i - distance in devices]
    return lax.ppermute(block, axis, route)


def with_halo(block, sides, width):
    for axis, dim in sides:
        count = lax.axis_size(axis)
        forward = [(i, i + 1) for i in range(count - 1)]
        backward = [(target, source) for source, target in forward]
        low = lax.ppermute(
            lax.slice_in_dim(block, block.shape[dim] - width, None, axis=dim), axis, forward
        )
        high = lax.ppermute(lax.slice_in_dim(block, 0, width, axis=dim), axis, backward)
        block = jnp.concatenate([low, block, high], axis=dim)
    return block


def rotate(projected, offset_pos):
    length, columns = projected.shape
    heads = columns // HEAD_DIM
    half = HEAD_DIM // 2
    positions = (offset_pos + jnp.arange(length)).astype(jnp.float32)
    inverse = 1.0 / 10000.0 ** (jnp.arange(half, dtype=jnp.float32) * 2.0 / HEAD_DIM)
    angles = positions[:, None] * inverse[None, :]
    angles = jnp.concatenate([angles, angles], axis=-1)
    cosine_table = jnp.cos(angles)[:, None, :]
    sine = jnp.sin(angles)[:, None, :]
    shaped = projected.reshape(length, heads, HEAD_DIM)
    turned = jnp.concatenate([-shaped[..., half:], shaped[..., :half]], axis=-1)
    return (shaped * cosine_table + turned * sine).reshape(length, columns)


def banded(queries, key_ext, value_ext, dilation, offset_pos, seq_len):
    length, columns = queries.shape
    heads = columns // HEAD_DIM
    class_len = length // dilation
    block_len = math.gcd(SIDE_STEPS, class_len)
    blocks = class_len // block_len
    extra = 2 * SIDE_STEPS // block_len
    query_blocks = queries.reshape(blocks, block_len, dilation, heads, HEAD_DIM)
    key_blocks = key_ext.reshape(blocks + extra, block_len, dilation, heads, HEAD_DIM)
    value_blocks = value_ext.reshape(blocks + extra, block_len, dilation, heads, HEAD_DIM)
    key_win = jnp.concatenate(
        [key_blocks[shift_idx : shift_idx + blocks] for shift_idx in range(extra + 1)], axis=1
    )
    value_win = jnp.concatenate(
        [value_blocks[shift_idx : shift_idx + blocks] for shift_idx in range(extra + 1)], axis=1
    )
    scores = jnp.einsum(
        "bqrhe,bkrhe->brhqk", query_blocks, key_win, preferred_element_type=jnp.float32
    )
    scores = scores * HEAD_DIM ** (-0.5)
    width_keys = key_win.shape[1]
    relative = jnp.arange(width_keys)[None, :] - jnp.arange(block_len)[:, None]
    within = (relative >= 0) & (relative <= 2 * SIDE_STEPS)
    key_rows = jnp.arange(blocks)[:, None] * block_len + jnp.arange(width_keys)[None, :]
    spots = (
        offset_pos
        - SIDE_STEPS * dilation
        + dilation * key_rows[:, :, None]
        + jnp.arange(dilation)[None, None, :]
    )
    inside = (spots >= 0) & (spots < seq_len)
    allowed = within[None, None, None] & jnp.transpose(inside, (0, 2, 1))[:, :, None, None, :]
    scores = jnp.where(allowed, scores, -1e30)
    row_max = jnp.max(scores, axis=-1, keepdims=True)
    expo = jnp.exp(scores - row_max)
    denom = jnp.sum(expo, axis=-1)
    probs = expo.astype(jnp.bfloat16)
    summed = jnp.einsum("brhqk,bkrhe->bqrhe", probs, value_win, preferred_element_type=jnp.float32)
    group_out = summed / jnp.transpose(denom, (0, 3, 1, 2))[..., None]
    log_sum = row_max[..., 0] + jnp.log(denom)
    log_sum = jnp.transpose(log_sum, (0, 3, 1, 2)).reshape(length, heads)
    return (group_out.reshape(length, columns), log_sum)


def collect(own_block, needed, direction):
    collected = own_block[None]
    while collected.shape[0] < needed + 1:
        stride = collected.shape[0]
        to_send = min(stride, needed + 1 - stride)
        arrived = shifted(collected[:to_send], "sp", direction * stride)
        collected = jnp.concatenate([collected, arrived], axis=0)
    return collected[1:]


def per_device(tokens, query_weight, key_weight, value_weight, out_weight):
    length = tokens.shape[0]
    offset_pos = lax.axis_index("sp") * length
    seq_len = lax.axis_size("sp") * length
    group_dilations = (1, MIDDLE_DILATION, FAR_DILATION)
    query_list = []
    pairs = []
    for group_idx in range(3):
        queries = rotate(
            jnp.dot(tokens, query_weight[group_idx], preferred_element_type=jnp.float32), offset_pos
        )
        keys_here = rotate(
            jnp.dot(tokens, key_weight[group_idx], preferred_element_type=jnp.float32), offset_pos
        )
        values_here = jnp.dot(tokens, value_weight[group_idx], preferred_element_type=jnp.float32)
        query_list.append(queries.astype(jnp.bfloat16))
        pairs.append(
            jnp.stack([keys_here.astype(jnp.bfloat16), values_here.astype(jnp.bfloat16)], axis=0)
        )
    middle_span_length = SIDE_STEPS * MIDDLE_DILATION
    first_ext = with_halo(pairs[0], (("sp", 1),), SIDE_STEPS)
    middle_ext = with_halo(pairs[1], (("sp", 1),), middle_span_length)
    far_span_length = SIDE_STEPS * FAR_DILATION
    needed = -(-far_span_length // length)
    lower_blocks = collect(pairs[2], needed, 1)
    upper_blocks = collect(pairs[2], needed, -1)
    columns = pairs[2].shape[2]
    lower_flat = jnp.moveaxis(lower_blocks[::-1], 0, 1).reshape(2, needed * length, columns)
    upper_flat = jnp.moveaxis(upper_blocks, 0, 1).reshape(2, needed * length, columns)
    far_full = jnp.concatenate([lower_flat, pairs[2], upper_flat], axis=1)
    extended = (first_ext, middle_ext, far_full)
    outputs = []
    log_sums = []
    for group_idx in range(3):
        group_out, log_sum = banded(
            query_list[group_idx],
            extended[group_idx][0],
            extended[group_idx][1],
            group_dilations[group_idx],
            offset_pos,
            seq_len,
        )
        outputs.append(group_out)
        log_sums.append(log_sum)
    merge_w = jax.nn.softmax(jnp.stack(log_sums, axis=0), axis=0)
    heads = columns // HEAD_DIM
    stacked = jnp.stack(outputs, axis=0).reshape(3, length, heads, HEAD_DIM)
    merged = (
        jnp.sum(merge_w[..., None] * stacked, axis=0).reshape(length, columns).astype(jnp.bfloat16)
    )
    mixed = jnp.dot(
        lax.all_gather(merged, "tp", axis=1, tiled=True),
        out_weight,
        preferred_element_type=jnp.float32,
    )
    return mixed.astype(jnp.bfloat16)


def remote(src, dst, send_sem, recv_sem, axis, target):
    return pltpu.make_async_remote_copy(
        src_ref=src,
        dst_ref=dst,
        send_sem=send_sem,
        recv_sem=recv_sem,
        device_id={axis: target},
        device_id_type=MESH,
    )


def head_mask(columns, head):
    lane = lax.broadcasted_iota(jnp.int32, (1, columns), 1)
    return (lane // HEAD_DIM == head).astype(jnp.float32)


def attend(queries, keys, values, bias):
    rows, columns = queries.shape
    heads = columns // HEAD_DIM
    masks = [head_mask(columns, head) for head in range(heads)]
    stacked = jnp.concatenate([queries * mask.astype(jnp.bfloat16) for mask in masks], axis=0)
    scores = lax.dot_general(
        stacked, keys, (((1,), (1,)), ((), ())), preferred_element_type=jnp.float32
    )
    width = keys.shape[0]
    scores = (scores.reshape(heads, rows, width) + bias[None]).reshape(heads * rows, width)
    row_max = jnp.max(scores, axis=-1, keepdims=True)
    expo = jnp.exp(scores - row_max)
    denom = jnp.sum(expo, axis=-1, keepdims=True)
    summed = jnp.dot(expo.astype(jnp.bfloat16), values, preferred_element_type=jnp.float32)
    summed = summed / denom
    lse = row_max + jnp.log(denom)
    parts = [slice(head * rows, (head + 1) * rows) for head in range(heads)]
    out = sum(summed[part] * mask for part, mask in zip(parts, masks))
    return out, [lse[part] for part in parts]


def packed_lse(lses):
    heads = len(lses)
    lane = lax.broadcasted_iota(jnp.int32, (1, 128), 1)
    spread = sum(lse * (lane % heads == head).astype(jnp.float32) for head, lse in enumerate(lses))
    total = jnp.zeros_like(spread)
    for term in range(3):
        rounded = spread.astype(jnp.bfloat16).astype(jnp.float32)
        total = total + rounded * (lane // heads == term).astype(jnp.float32)
        spread = spread - rounded
    return total.astype(jnp.bfloat16)


def band_bias(rows, width, offset, low, high):
    query = lax.broadcasted_iota(jnp.int32, (rows, width), 0)
    key = lax.broadcasted_iota(jnp.int32, (rows, width), 1)
    step = key + offset - query
    keep = (step >= -SIDE_STEPS) & (step <= SIDE_STEPS) & (key >= low) & (key < high)
    return jnp.where(keep, 0.0, -1e30)


def permutation(length, dilation, inverse):
    row = lax.broadcasted_iota(jnp.int32, (length, length), 1 if inverse else 0)
    column = lax.broadcasted_iota(jnp.int32, (length, length), 0 if inverse else 1)
    steps = length // dilation
    source = (row % steps) * dilation + row // steps
    return (source == column).astype(jnp.float32).astype(jnp.bfloat16)


def fused_kernel(
    n, m, tokens_hbm, query_hbm, key_hbm, value_hbm, out_hbm, table_hbm, base_ref, result_ref,
    tokens, weights, out_weight, table, kv_first, kv_middle, far_send, far_recv,
    back_send, back_recv, merged_all, load_sem, weight_sem, local_sem,
    near_send_sem, near_recv_sem, far_send_sem, far_recv_sem, back_send_sem, back_recv_sem,
    tp_send_sem, tp_recv_sem,
):
    me = lax.axis_index("sp")
    mine = lax.axis_index("tp")
    length, columns = tokens.shape[0], weights.shape[-1]
    half = HEAD_DIM // 2
    classes = FAR_DILATION // n
    halo = SIDE_STEPS

    loads = [
        pltpu.make_async_copy(tokens_hbm, tokens, load_sem.at[0]),
        pltpu.make_async_copy(table_hbm, table, load_sem.at[1]),
        pltpu.make_async_copy(out_hbm, out_weight, load_sem.at[2]),
    ]
    weight_loads = {}
    for group in (2, 1, 0):
        for kind, source in ((1, key_hbm), (2, value_hbm), (0, query_hbm)):
            slot = group * 3 + kind
            weight_loads[group, kind] = pltpu.make_async_copy(
                source.at[group], weights.at[slot], weight_sem.at[slot]
            )
    loads[0].start()
    loads[1].start()
    for kind in (1, 2, 0):
        weight_loads[2, kind].start()
    later_loads = [weight_loads[group, kind] for group in (1, 0) for kind in (1, 2)]
    later_loads += [weight_loads[1, 0], weight_loads[0, 0], loads[2]]

    barrier = pltpu.get_barrier_semaphore()
    for distance in range(1, n):
        pl.semaphore_signal(
            barrier, inc=1, device_id={"sp": lax.rem(me + distance, n)}, device_id_type=MESH
        )
    for distance in range(1, m):
        pl.semaphore_signal(
            barrier, inc=1, device_id={"tp": lax.rem(mine + distance, m)}, device_id_type=MESH
        )

    @pl.when(me == 0)
    def _():
        kv_first[:, :halo] = jnp.zeros((2, halo, columns), jnp.bfloat16)
        kv_middle[:, :, 0] = jnp.zeros_like(kv_middle[:, :, 0])

    @pl.when(me == n - 1)
    def _():
        kv_first[:, halo + length :] = jnp.zeros((2, halo, columns), jnp.bfloat16)
        kv_middle[:, :, 2] = jnp.zeros_like(kv_middle[:, :, 2])

    loads[1].wait()
    base_cos = base_ref[0, pl.ds(me, 1), :]
    base_sin = base_ref[1, pl.ds(me, 1), :]
    cosine = base_cos * table[0] - base_sin * table[1]
    sine = base_sin * table[0] + base_cos * table[1]
    wide = columns // cosine.shape[1]
    lane = lax.broadcasted_iota(jnp.int32, (1, columns), 1)
    first_half = lane % HEAD_DIM < half
    cosine = jnp.concatenate([cosine] * wide, axis=1)
    sine = jnp.concatenate([sine] * wide, axis=1) * jnp.where(first_half, -1.0, 1.0)
    far_order = permutation(length, FAR_DILATION, False)
    middle_order = permutation(length, MIDDLE_DILATION, False)
    loads[0].wait()

    def project(group, kind):
        weight_loads[group, kind].wait()
        product = jnp.dot(
            tokens[...], weights[group * 3 + kind], preferred_element_type=jnp.float32
        )
        if kind < 2:
            later = pltpu.roll(product, columns - half, 1)
            earlier = pltpu.roll(product, half, 1)
            product = product * cosine + jnp.where(first_half, later, earlier) * sine
        if kind == 0:
            product = product * HEAD_DIM ** (-0.5)
        return product.astype(jnp.bfloat16)

    def ordered(order, block):
        return jnp.dot(order, block, preferred_element_type=jnp.float32).astype(jnp.bfloat16)

    far_copies = []
    for kind in (1, 2, 0):
        far_send[kind] = ordered(far_order, project(2, kind)).reshape(far_send.shape[1:])
        for load in later_loads[:3]:
            load.start()
        later_loads = later_loads[3:]
        if kind == 1:
            pl.semaphore_wait(barrier, n - 1 + m - 1)
        for distance in range(1, n):
            target = lax.rem(me + distance, n)
            copy = remote(
                far_send.at[kind, pl.ds(target * classes, classes)],
                far_recv.at[kind, :, me],
                far_send_sem.at[kind, distance],
                far_recv_sem.at[kind, distance],
                "sp",
                target,
            )
            copy.start()
            far_copies.append(copy)
    far_own = pltpu.make_async_copy(
        far_send.at[:, pl.ds(me * classes, classes)], far_recv.at[:, :, me], local_sem.at[0]
    )
    far_own.start()

    for kind in (1, 2):
        kv_middle[kind - 1, :, 1] = ordered(middle_order, project(1, kind)).reshape(
            MIDDLE_DILATION, length // MIDDLE_DILATION, columns
        )
    middle_up = remote(
        kv_middle.at[:, :, 1], kv_middle.at[:, :, 0],
        near_send_sem.at[0], near_recv_sem.at[0], "sp", lax.rem(me + 1, n),
    )
    middle_down = remote(
        kv_middle.at[:, :, 1], kv_middle.at[:, :, 2],
        near_send_sem.at[1], near_recv_sem.at[1], "sp", lax.rem(me + n - 1, n),
    )
    first_up = remote(
        kv_first.at[:, pl.ds(length, halo)], kv_first.at[:, pl.ds(0, halo)],
        near_send_sem.at[2], near_recv_sem.at[2], "sp", lax.rem(me + 1, n),
    )
    first_down = remote(
        kv_first.at[:, pl.ds(halo, halo)], kv_first.at[:, pl.ds(halo + length, halo)],
        near_send_sem.at[3], near_recv_sem.at[3], "sp", lax.rem(me + n - 1, n),
    )

    @pl.when(me < n - 1)
    def _():
        middle_up.start()

    @pl.when(me > 0)
    def _():
        middle_down.start()

    for kind in (1, 2):
        kv_first[kind - 1, halo : halo + length] = project(0, kind)

    @pl.when(me < n - 1)
    def _():
        first_up.start()

    @pl.when(me > 0)
    def _():
        first_down.start()

    middle_queries = ordered(middle_order, project(1, 0))
    first_queries = project(0, 0)

    far_own.wait()
    for copy in far_copies:
        copy.wait()
    class_len = n * (length // FAR_DILATION)
    far_bias = band_bias(class_len, class_len, 0, 0, class_len)
    for index in range(classes):
        queries, keys, values = (
            far_recv[kind, index].reshape(class_len, columns) for kind in range(3)
        )
        out, lses = attend(queries, keys, values, far_bias)
        back_send[index, :, :, :columns] = out.astype(jnp.bfloat16).reshape(n, -1, columns)
        back_send[index, :, :, columns:] = packed_lse(lses).reshape(n, -1, 128)
    back_copies = []
    for distance in range(1, n):
        target = lax.rem(me + distance, n)
        copy = remote(
            back_send.at[:, target],
            back_recv.at[pl.ds(me * classes, classes)],
            back_send_sem.at[distance],
            back_recv_sem.at[distance],
            "sp",
            target,
        )
        copy.start()
        back_copies.append(copy)
    back_own = pltpu.make_async_copy(
        back_send.at[:, me], back_recv.at[pl.ds(me * classes, classes)], local_sem.at[1]
    )
    back_own.start()

    @pl.when(me < n - 1)
    def _():
        first_up.wait_send()
        first_down.wait_recv()

    @pl.when(me > 0)
    def _():
        first_down.wait_send()
        first_up.wait_recv()

    tile = 2 * halo
    first_outs = []
    first_lses = []
    for start in range(0, length, tile):
        width = tile + 2 * halo
        low = halo - start - me * length
        high = halo - start + (n - me) * length
        out, lses = attend(
            first_queries[start : start + tile],
            kv_first[0, start : start + width],
            kv_first[1, start : start + width],
            band_bias(tile, width, -halo, low, high),
        )
        first_outs.append(out)
        first_lses.append(
            sum(lse * head_mask(columns, head) for head, lse in enumerate(lses))
        )
    first_out = jnp.concatenate(first_outs, axis=0)
    first_lse = jnp.concatenate(first_lses, axis=0)

    @pl.when(me < n - 1)
    def _():
        middle_up.wait_send()
        middle_down.wait_recv()

    @pl.when(me > 0)
    def _():
        middle_down.wait_send()
        middle_up.wait_recv()

    steps = length // MIDDLE_DILATION
    low = jnp.where(me == 0, steps, 0)
    high = jnp.where(me == n - 1, 2 * steps, 3 * steps)
    middle_bias = band_bias(steps, 3 * steps, -steps, low, high)
    middle_parts = []
    for index in range(MIDDLE_DILATION):
        out, lses = attend(
            middle_queries[index * steps : (index + 1) * steps],
            kv_middle[0, index].reshape(3 * steps, columns),
            kv_middle[1, index].reshape(3 * steps, columns),
            middle_bias,
        )
        middle_parts.append(
            jnp.concatenate([out.astype(jnp.bfloat16), packed_lse(lses)], axis=1)
        )

    heads = columns // HEAD_DIM
    term = lax.broadcasted_iota(jnp.int32, (128, columns), 0)
    column = lax.broadcasted_iota(jnp.int32, (128, columns), 1)
    spread = (term % heads == column // HEAD_DIM) & (term < 3 * heads)
    spread = spread.astype(jnp.float32).astype(jnp.bfloat16)

    def natural(dilation, block):
        block = jnp.dot(
            permutation(length, dilation, True), block, preferred_element_type=jnp.float32
        )
        lse = jnp.dot(
            block[:, columns:].astype(jnp.bfloat16), spread, preferred_element_type=jnp.float32
        )
        return block[:, :columns], lse

    middle_out, middle_lse = natural(MIDDLE_DILATION, jnp.concatenate(middle_parts, axis=0))

    back_own.wait()
    for copy in back_copies:
        copy.wait()
    far_out, far_lse = natural(
        FAR_DILATION, back_recv[...].reshape(length, back_recv.shape[2])
    )

    top = jnp.maximum(jnp.maximum(first_lse, middle_lse), far_lse)
    first_w = jnp.exp(first_lse - top)
    middle_w = jnp.exp(middle_lse - top)
    far_w = jnp.exp(far_lse - top)
    merged = (first_w * first_out + middle_w * middle_out + far_w * far_out) / (
        first_w + middle_w + far_w
    )
    merged_all[0] = merged.astype(jnp.bfloat16)

    chips = m // 2
    sibling = mine + 1 - 2 * lax.rem(mine, 2)
    piece = length // 2

    def hand(part, source, slot, target):
        rows = pl.ds(part * piece, piece)
        copy = remote(
            merged_all.at[source, rows],
            merged_all.at[slot, rows],
            tp_send_sem.at[part, slot],
            tp_recv_sem.at[part, slot],
            "tp",
            target,
        )
        copy.start()
        return copy

    copies = {}
    for part in range(2):
        for chip in range(1, chips):
            copies[part, chip] = hand(part, 0, chip, lax.rem(mine + 2 * chip, m))
    for part in range(2):
        copies[part, chips] = hand(part, 0, chips, sibling)
    loads[2].wait()

    def term(part, slot):
        chip = slot % chips
        owner = lax.rem((mine if slot < chips else sibling) - 2 * chip + m, m)
        rows = pl.ds(pl.multiple_of(owner * columns, columns), columns)
        return jnp.dot(
            merged_all[slot, part * piece : (part + 1) * piece],
            out_weight[rows, :],
            preferred_element_type=jnp.float32,
        )

    totals = [term(part, 0) for part in range(2)]
    for part in range(2):
        for chip in range(1, chips):
            copies[part, chip].wait()
            copies[part, chips + chip] = hand(part, chip, chips + chip, sibling)
        copies[part, chips].wait()
        totals[part] = totals[part] + term(part, chips)
        for chip in range(1, chips):
            totals[part] = totals[part] + term(part, chip)
    for part in range(2):
        for chip in range(1, chips):
            copies[part, chips + chip].wait()
            totals[part] = totals[part] + term(part, chips + chip)
        result_ref[part * piece : (part + 1) * piece] = totals[part].astype(result_ref.dtype)


def turn_tables(n, length):
    half = HEAD_DIM // 2
    inverse = 1.0 / 10000.0 ** (np.arange(half, dtype=np.float32) * np.float32(2.0) / HEAD_DIM)
    inverse = np.tile(inverse.astype(np.float64), 128 // half)[None]
    inner = np.arange(length)[:, None] * inverse
    outer = (np.arange(n) * length)[:, None] * inverse
    table = np.stack([np.cos(inner), np.sin(inner)]).astype(np.float32)
    base = np.stack([np.cos(outer), np.sin(outer)]).astype(np.float32)
    return table, base


def fused(n, m, tokens, query_weight, key_weight, value_weight, out_weight):
    length, width = tokens.shape
    columns = query_weight.shape[2]
    table, base = turn_tables(n, length)
    steps = length // FAR_DILATION
    classes = FAR_DILATION // n
    kept = columns + 128
    bf16 = jnp.bfloat16
    hbm = pl.BlockSpec(memory_space=pl.ANY)
    vmem = pl.BlockSpec(memory_space=pltpu.VMEM)
    dma = pltpu.SemaphoreType.DMA
    return pl.pallas_call(
        functools.partial(fused_kernel, n, m),
        out_shape=jax.ShapeDtypeStruct((length, out_weight.shape[1]), jnp.float32),
        in_specs=[hbm] * 6 + [vmem],
        out_specs=vmem,
        scratch_shapes=[
            pltpu.VMEM((length, width), bf16),
            pltpu.VMEM((9, width, columns), bf16),
            pltpu.VMEM(out_weight.shape, bf16),
            pltpu.VMEM(table.shape, jnp.float32),
            pltpu.VMEM((2, length + 2 * SIDE_STEPS, columns), bf16),
            pltpu.VMEM((2, MIDDLE_DILATION, 3, length // MIDDLE_DILATION, columns), bf16),
            pltpu.VMEM((3, FAR_DILATION, steps, columns), bf16),
            pltpu.VMEM((3, classes, n, steps, columns), bf16),
            pltpu.VMEM((classes, n, steps, kept), bf16),
            pltpu.VMEM((FAR_DILATION, steps, kept), bf16),
            pltpu.VMEM((m, length, columns), bf16),
            dma((3,)),
            dma((9,)),
            dma((2,)),
            dma((4,)),
            dma((4,)),
            dma((3, n)),
            dma((3, n)),
            dma((n,)),
            dma((n,)),
            dma((2, m)),
            dma((2, m)),
        ],
        compiler_params=pltpu.CompilerParams(
            collective_id=0, has_side_effects=True, vmem_limit_bytes=60 * 1024 * 1024
        ),
    )(tokens, query_weight, key_weight, value_weight, out_weight, jnp.asarray(table), jnp.asarray(base)).astype(bf16)


def planned(n, m, *arrays):
    length, columns = arrays[0].shape[0], arrays[1].shape[2]
    fits = (
        n > 1
        and m % 2 == 0
        and FAR_DILATION % n == 0
        and length == SIDE_STEPS * MIDDLE_DILATION
        and length % (FAR_DILATION * 16) == 0
        and columns % 128 == 0
        and 3 * (columns // HEAD_DIM) <= 128
    )
    if fits:
        return fused(n, m, *arrays)
    return per_device(*arrays)


def solution(mesh):
    placed = (
        P("sp", None),
        P(None, None, "tp"),
        P(None, None, "tp"),
        P(None, None, "tp"),
        P(None, "tp"),
    )
    return jax.shard_map(
        functools.partial(planned, mesh.shape["sp"], mesh.shape["tp"]),
        mesh=mesh,
        in_specs=placed,
        out_specs=P("sp", "tp"),
        check_vma=False,
    )
```

```python
import functools
import math

import jax
import numpy as np
import jax.numpy as jnp
from jax import lax
from jax.experimental import pallas as pl
from jax.experimental.pallas import tpu as pltpu
from jax.sharding import PartitionSpec as P

HEAD_DIM = 64
SIDE_STEPS = 64
MIDDLE_DILATION = 4
FAR_DILATION = 16
MESH = pl.DeviceIdType.MESH


def shifted(block, axis, distance):
    devices = range(lax.axis_size(axis))
    route = [(i - distance, i) for i in devices if i - distance in devices]
    return lax.ppermute(block, axis, route)


def with_halo(block, sides, width):
    for axis, dim in sides:
        count = lax.axis_size(axis)
        forward = [(i, i + 1) for i in range(count - 1)]
        backward = [(target, source) for source, target in forward]
        low = lax.ppermute(
            lax.slice_in_dim(block, block.shape[dim] - width, None, axis=dim), axis, forward
        )
        high = lax.ppermute(lax.slice_in_dim(block, 0, width, axis=dim), axis, backward)
        block = jnp.concatenate([low, block, high], axis=dim)
    return block


def rotate(projected, offset_pos):
    length, columns = projected.shape
    heads = columns // HEAD_DIM
    half = HEAD_DIM // 2
    positions = (offset_pos + jnp.arange(length)).astype(jnp.float32)
    inverse = 1.0 / 10000.0 ** (jnp.arange(half, dtype=jnp.float32) * 2.0 / HEAD_DIM)
    angles = positions[:, None] * inverse[None, :]
    angles = jnp.concatenate([angles, angles], axis=-1)
    cosine_table = jnp.cos(angles)[:, None, :]
    sine = jnp.sin(angles)[:, None, :]
    shaped = projected.reshape(length, heads, HEAD_DIM)
    turned = jnp.concatenate([-shaped[..., half:], shaped[..., :half]], axis=-1)
    return (shaped * cosine_table + turned * sine).reshape(length, columns)


def banded(queries, key_ext, value_ext, dilation, offset_pos, seq_len):
    length, columns = queries.shape
    heads = columns // HEAD_DIM
    class_len = length // dilation
    block_len = math.gcd(SIDE_STEPS, class_len)
    blocks = class_len // block_len
    extra = 2 * SIDE_STEPS // block_len
    query_blocks = queries.reshape(blocks, block_len, dilation, heads, HEAD_DIM)
    key_blocks = key_ext.reshape(blocks + extra, block_len, dilation, heads, HEAD_DIM)
    value_blocks = value_ext.reshape(blocks + extra, block_len, dilation, heads, HEAD_DIM)
    key_win = jnp.concatenate(
        [key_blocks[shift_idx : shift_idx + blocks] for shift_idx in range(extra + 1)], axis=1
    )
    value_win = jnp.concatenate(
        [value_blocks[shift_idx : shift_idx + blocks] for shift_idx in range(extra + 1)], axis=1
    )
    scores = jnp.einsum(
        "bqrhe,bkrhe->brhqk", query_blocks, key_win, preferred_element_type=jnp.float32
    )
    scores = scores * HEAD_DIM ** (-0.5)
    width_keys = key_win.shape[1]
    relative = jnp.arange(width_keys)[None, :] - jnp.arange(block_len)[:, None]
    within = (relative >= 0) & (relative <= 2 * SIDE_STEPS)
    key_rows = jnp.arange(blocks)[:, None] * block_len + jnp.arange(width_keys)[None, :]
    spots = (
        offset_pos
        - SIDE_STEPS * dilation
        + dilation * key_rows[:, :, None]
        + jnp.arange(dilation)[None, None, :]
    )
    inside = (spots >= 0) & (spots < seq_len)
    allowed = within[None, None, None] & jnp.transpose(inside, (0, 2, 1))[:, :, None, None, :]
    scores = jnp.where(allowed, scores, -1e30)
    row_max = jnp.max(scores, axis=-1, keepdims=True)
    expo = jnp.exp(scores - row_max)
    denom = jnp.sum(expo, axis=-1)
    probs = expo.astype(jnp.bfloat16)
    summed = jnp.einsum("brhqk,bkrhe->bqrhe", probs, value_win, preferred_element_type=jnp.float32)
    group_out = summed / jnp.transpose(denom, (0, 3, 1, 2))[..., None]
    log_sum = row_max[..., 0] + jnp.log(denom)
    log_sum = jnp.transpose(log_sum, (0, 3, 1, 2)).reshape(length, heads)
    return (group_out.reshape(length, columns), log_sum)


def collect(own_block, needed, direction):
    collected = own_block[None]
    while collected.shape[0] < needed + 1:
        stride = collected.shape[0]
        to_send = min(stride, needed + 1 - stride)
        arrived = shifted(collected[:to_send], "sp", direction * stride)
        collected = jnp.concatenate([collected, arrived], axis=0)
    return collected[1:]


def per_device(tokens, query_weight, key_weight, value_weight, out_weight):
    length = tokens.shape[0]
    offset_pos = lax.axis_index("sp") * length
    seq_len = lax.axis_size("sp") * length
    group_dilations = (1, MIDDLE_DILATION, FAR_DILATION)
    query_list = []
    pairs = []
    for group_idx in range(3):
        queries = rotate(
            jnp.dot(tokens, query_weight[group_idx], preferred_element_type=jnp.float32), offset_pos
        )
        keys_here = rotate(
            jnp.dot(tokens, key_weight[group_idx], preferred_element_type=jnp.float32), offset_pos
        )
        values_here = jnp.dot(tokens, value_weight[group_idx], preferred_element_type=jnp.float32)
        query_list.append(queries.astype(jnp.bfloat16))
        pairs.append(
            jnp.stack([keys_here.astype(jnp.bfloat16), values_here.astype(jnp.bfloat16)], axis=0)
        )
    middle_span_length = SIDE_STEPS * MIDDLE_DILATION
    first_ext = with_halo(pairs[0], (("sp", 1),), SIDE_STEPS)
    middle_ext = with_halo(pairs[1], (("sp", 1),), middle_span_length)
    far_span_length = SIDE_STEPS * FAR_DILATION
    needed = -(-far_span_length // length)
    lower_blocks = collect(pairs[2], needed, 1)
    upper_blocks = collect(pairs[2], needed, -1)
    columns = pairs[2].shape[2]
    lower_flat = jnp.moveaxis(lower_blocks[::-1], 0, 1).reshape(2, needed * length, columns)
    upper_flat = jnp.moveaxis(upper_blocks, 0, 1).reshape(2, needed * length, columns)
    far_full = jnp.concatenate([lower_flat, pairs[2], upper_flat], axis=1)
    extended = (first_ext, middle_ext, far_full)
    outputs = []
    log_sums = []
    for group_idx in range(3):
        group_out, log_sum = banded(
            query_list[group_idx],
            extended[group_idx][0],
            extended[group_idx][1],
            group_dilations[group_idx],
            offset_pos,
            seq_len,
        )
        outputs.append(group_out)
        log_sums.append(log_sum)
    merge_w = jax.nn.softmax(jnp.stack(log_sums, axis=0), axis=0)
    heads = columns // HEAD_DIM
    stacked = jnp.stack(outputs, axis=0).reshape(3, length, heads, HEAD_DIM)
    merged = (
        jnp.sum(merge_w[..., None] * stacked, axis=0).reshape(length, columns).astype(jnp.bfloat16)
    )
    mixed = jnp.dot(
        lax.all_gather(merged, "tp", axis=1, tiled=True),
        out_weight,
        preferred_element_type=jnp.float32,
    )
    return mixed.astype(jnp.bfloat16)


def remote(src, dst, send_sem, recv_sem, axis, target):
    return pltpu.make_async_remote_copy(
        src_ref=src,
        dst_ref=dst,
        send_sem=send_sem,
        recv_sem=recv_sem,
        device_id={axis: target},
        device_id_type=MESH,
    )


def head_mask(columns, head):
    lane = lax.broadcasted_iota(jnp.int32, (1, columns), 1)
    return (lane // HEAD_DIM == head).astype(jnp.float32)


def attend(queries, keys, values, bias):
    rows, columns = queries.shape
    heads = columns // HEAD_DIM
    masks = [head_mask(columns, head) for head in range(heads)]
    stacked = jnp.concatenate([queries * mask.astype(jnp.bfloat16) for mask in masks], axis=0)
    scores = lax.dot_general(
        stacked, keys, (((1,), (1,)), ((), ())), preferred_element_type=jnp.float32
    )
    width = keys.shape[0]
    scores = (scores.reshape(heads, rows, width) + bias[None]).reshape(heads * rows, width)
    row_max = jnp.max(scores, axis=-1, keepdims=True)
    expo = jnp.exp(scores - row_max)
    denom = jnp.sum(expo, axis=-1, keepdims=True)
    summed = jnp.dot(expo.astype(jnp.bfloat16), values, preferred_element_type=jnp.float32)
    summed = summed / denom
    lse = row_max + jnp.log(denom)
    parts = [slice(head * rows, (head + 1) * rows) for head in range(heads)]
    out = sum(summed[part] * mask for part, mask in zip(parts, masks))
    return out, [lse[part] for part in parts]


def packed_lse(lses):
    heads = len(lses)
    lane = lax.broadcasted_iota(jnp.int32, (1, 128), 1)
    spread = sum(lse * (lane % heads == head).astype(jnp.float32) for head, lse in enumerate(lses))
    total = jnp.zeros_like(spread)
    for term in range(3):
        rounded = spread.astype(jnp.bfloat16).astype(jnp.float32)
        total = total + rounded * (lane // heads == term).astype(jnp.float32)
        spread = spread - rounded
    return total.astype(jnp.bfloat16)


def band_bias(rows, width, offset, low, high):
    query = lax.broadcasted_iota(jnp.int32, (rows, width), 0)
    key = lax.broadcasted_iota(jnp.int32, (rows, width), 1)
    step = key + offset - query
    keep = (step >= -SIDE_STEPS) & (step <= SIDE_STEPS) & (key >= low) & (key < high)
    return jnp.where(keep, 0.0, -1e30)


def permutation(length, dilation, inverse):
    row = lax.broadcasted_iota(jnp.int32, (length, length), 1 if inverse else 0)
    column = lax.broadcasted_iota(jnp.int32, (length, length), 0 if inverse else 1)
    steps = length // dilation
    source = (row % steps) * dilation + row // steps
    return (source == column).astype(jnp.float32).astype(jnp.bfloat16)


def fused_kernel(
    n, m, tokens_hbm, query_hbm, key_hbm, value_hbm, out_hbm, table_hbm, base_ref, result_ref,
    tokens, weights, out_weight, table, kv_first, kv_middle, far_send, far_recv,
    back_send, back_recv, merged_all, load_sem, weight_sem, local_sem,
    near_send_sem, near_recv_sem, far_send_sem, far_recv_sem, back_send_sem, back_recv_sem,
    tp_send_sem, tp_recv_sem,
):
    me = lax.axis_index("sp")
    mine = lax.axis_index("tp")
    length, columns = tokens.shape[0], weights.shape[-1]
    half = HEAD_DIM // 2
    classes = FAR_DILATION // n
    halo = SIDE_STEPS

    loads = [
        pltpu.make_async_copy(tokens_hbm, tokens, load_sem.at[0]),
        pltpu.make_async_copy(table_hbm, table, load_sem.at[1]),
        pltpu.make_async_copy(out_hbm, out_weight, load_sem.at[2]),
    ]
    weight_loads = {}
    for group in (2, 1, 0):
        for kind, source in ((1, key_hbm), (2, value_hbm), (0, query_hbm)):
            slot = group * 3 + kind
            weight_loads[group, kind] = pltpu.make_async_copy(
                source.at[group], weights.at[slot], weight_sem.at[slot]
            )
    loads[0].start()
    loads[1].start()
    for kind in (1, 2, 0):
        weight_loads[2, kind].start()
    later_loads = [weight_loads[group, kind] for group in (0, 1) for kind in (1, 2)]
    later_loads += [weight_loads[1, 0], weight_loads[0, 0], loads[2]]

    barrier = pltpu.get_barrier_semaphore()
    for distance in range(1, n):
        pl.semaphore_signal(
            barrier, inc=1, device_id={"sp": lax.rem(me + distance, n)}, device_id_type=MESH
        )
    for distance in range(1, m):
        pl.semaphore_signal(
            barrier, inc=1, device_id={"tp": lax.rem(mine + distance, m)}, device_id_type=MESH
        )

    @pl.when(me == 0)
    def _():
        kv_first[:, :halo] = jnp.zeros((2, halo, columns), jnp.bfloat16)
        kv_middle[:, :, 0] = jnp.zeros_like(kv_middle[:, :, 0])

    @pl.when(me == n - 1)
    def _():
        kv_first[:, halo + length :] = jnp.zeros((2, halo, columns), jnp.bfloat16)
        kv_middle[:, :, 2] = jnp.zeros_like(kv_middle[:, :, 2])

    loads[1].wait()
    base_cos = base_ref[0, pl.ds(me, 1), :]
    base_sin = base_ref[1, pl.ds(me, 1), :]
    cosine = base_cos * table[0] - base_sin * table[1]
    sine = base_sin * table[0] + base_cos * table[1]
    wide = columns // cosine.shape[1]
    lane = lax.broadcasted_iota(jnp.int32, (1, columns), 1)
    first_half = lane % HEAD_DIM < half
    cosine = jnp.concatenate([cosine] * wide, axis=1)
    sine = jnp.concatenate([sine] * wide, axis=1) * jnp.where(first_half, -1.0, 1.0)
    far_order = permutation(length, FAR_DILATION, False)
    middle_order = permutation(length, MIDDLE_DILATION, False)
    loads[0].wait()

    def project(group, kind):
        weight_loads[group, kind].wait()
        product = jnp.dot(
            tokens[...], weights[group * 3 + kind], preferred_element_type=jnp.float32
        )
        if kind < 2:
            later = pltpu.roll(product, columns - half, 1)
            earlier = pltpu.roll(product, half, 1)
            product = product * cosine + jnp.where(first_half, later, earlier) * sine
        if kind == 0:
            product = product * HEAD_DIM ** (-0.5)
        return product.astype(jnp.bfloat16)

    def ordered(order, block):
        return jnp.dot(order, block, preferred_element_type=jnp.float32).astype(jnp.bfloat16)

    far_copies = []
    for kind in (1, 2, 0):
        far_send[kind] = ordered(far_order, project(2, kind)).reshape(far_send.shape[1:])
        for load in later_loads[:3]:
            load.start()
        later_loads = later_loads[3:]
        if kind == 1:
            pl.semaphore_wait(barrier, n - 1 + m - 1)
        for distance in range(1, n):
            target = lax.rem(me + distance, n)
            copy = remote(
                far_send.at[kind, pl.ds(target * classes, classes)],
                far_recv.at[kind, :, me],
                far_send_sem.at[kind, distance],
                far_recv_sem.at[kind, distance],
                "sp",
                target,
            )
            copy.start()
            far_copies.append(copy)
    far_own = pltpu.make_async_copy(
        far_send.at[:, pl.ds(me * classes, classes)], far_recv.at[:, :, me], local_sem.at[0]
    )
    far_own.start()

    middle_up = remote(
        kv_middle.at[:, :, 1], kv_middle.at[:, :, 0],
        near_send_sem.at[0], near_recv_sem.at[0], "sp", lax.rem(me + 1, n),
    )
    middle_down = remote(
        kv_middle.at[:, :, 1], kv_middle.at[:, :, 2],
        near_send_sem.at[1], near_recv_sem.at[1], "sp", lax.rem(me + n - 1, n),
    )
    first_up = remote(
        kv_first.at[:, pl.ds(length, halo)], kv_first.at[:, pl.ds(0, halo)],
        near_send_sem.at[2], near_recv_sem.at[2], "sp", lax.rem(me + 1, n),
    )
    first_down = remote(
        kv_first.at[:, pl.ds(halo, halo)], kv_first.at[:, pl.ds(halo + length, halo)],
        near_send_sem.at[3], near_recv_sem.at[3], "sp", lax.rem(me + n - 1, n),
    )

    for kind in (1, 2):
        kv_first[kind - 1, halo : halo + length] = project(0, kind)

    @pl.when(me < n - 1)
    def _():
        first_up.start()

    @pl.when(me > 0)
    def _():
        first_down.start()

    for kind in (1, 2):
        kv_middle[kind - 1, :, 1] = ordered(middle_order, project(1, kind)).reshape(
            MIDDLE_DILATION, length // MIDDLE_DILATION, columns
        )
    @pl.when(me < n - 1)
    def _():
        middle_up.start()

    @pl.when(me > 0)
    def _():
        middle_down.start()

    middle_queries = ordered(middle_order, project(1, 0))
    first_queries = project(0, 0)

    far_own.wait()
    for copy in far_copies:
        copy.wait()
    class_len = n * (length // FAR_DILATION)
    far_bias = band_bias(class_len, class_len, 0, 0, class_len)
    for index in range(classes):
        queries, keys, values = (
            far_recv[kind, index].reshape(class_len, columns) for kind in range(3)
        )
        out, lses = attend(queries, keys, values, far_bias)
        back_send[index, :, :, :columns] = out.astype(jnp.bfloat16).reshape(n, -1, columns)
        back_send[index, :, :, columns:] = packed_lse(lses).reshape(n, -1, 128)
    back_copies = []
    for distance in range(1, n):
        target = lax.rem(me + distance, n)
        copy = remote(
            back_send.at[:, target],
            back_recv.at[pl.ds(me * classes, classes)],
            back_send_sem.at[distance],
            back_recv_sem.at[distance],
            "sp",
            target,
        )
        copy.start()
        back_copies.append(copy)
    back_own = pltpu.make_async_copy(
        back_send.at[:, me], back_recv.at[pl.ds(me * classes, classes)], local_sem.at[1]
    )
    back_own.start()

    @pl.when(me < n - 1)
    def _():
        first_up.wait_send()
        first_down.wait_recv()

    @pl.when(me > 0)
    def _():
        first_down.wait_send()
        first_up.wait_recv()

    tile = 2 * halo
    first_outs = []
    first_lses = []
    for start in range(0, length, tile):
        width = tile + 2 * halo
        low = halo - start - me * length
        high = halo - start + (n - me) * length
        out, lses = attend(
            first_queries[start : start + tile],
            kv_first[0, start : start + width],
            kv_first[1, start : start + width],
            band_bias(tile, width, -halo, low, high),
        )
        first_outs.append(out)
        first_lses.append(
            sum(lse * head_mask(columns, head) for head, lse in enumerate(lses))
        )
    first_out = jnp.concatenate(first_outs, axis=0)
    first_lse = jnp.concatenate(first_lses, axis=0)

    @pl.when(me < n - 1)
    def _():
        middle_up.wait_send()
        middle_down.wait_recv()

    @pl.when(me > 0)
    def _():
        middle_down.wait_send()
        middle_up.wait_recv()

    steps = length // MIDDLE_DILATION
    low = jnp.where(me == 0, steps, 0)
    high = jnp.where(me == n - 1, 2 * steps, 3 * steps)
    middle_bias = band_bias(steps, 3 * steps, -steps, low, high)
    middle_parts = []
    for index in range(MIDDLE_DILATION):
        out, lses = attend(
            middle_queries[index * steps : (index + 1) * steps],
            kv_middle[0, index].reshape(3 * steps, columns),
            kv_middle[1, index].reshape(3 * steps, columns),
            middle_bias,
        )
        middle_parts.append(
            jnp.concatenate([out.astype(jnp.bfloat16), packed_lse(lses)], axis=1)
        )

    heads = columns // HEAD_DIM
    term = lax.broadcasted_iota(jnp.int32, (128, columns), 0)
    column = lax.broadcasted_iota(jnp.int32, (128, columns), 1)
    spread = (term % heads == column // HEAD_DIM) & (term < 3 * heads)
    spread = spread.astype(jnp.float32).astype(jnp.bfloat16)

    def natural(dilation, block):
        block = jnp.dot(
            permutation(length, dilation, True), block, preferred_element_type=jnp.float32
        )
        lse = jnp.dot(
            block[:, columns:].astype(jnp.bfloat16), spread, preferred_element_type=jnp.float32
        )
        return block[:, :columns], lse

    middle_out, middle_lse = natural(MIDDLE_DILATION, jnp.concatenate(middle_parts, axis=0))

    back_own.wait()
    for copy in back_copies:
        copy.wait()
    far_out, far_lse = natural(
        FAR_DILATION, back_recv[...].reshape(length, back_recv.shape[2])
    )

    top = jnp.maximum(jnp.maximum(first_lse, middle_lse), far_lse)
    first_w = jnp.exp(first_lse - top)
    middle_w = jnp.exp(middle_lse - top)
    far_w = jnp.exp(far_lse - top)
    merged = (first_w * first_out + middle_w * middle_out + far_w * far_out) / (
        first_w + middle_w + far_w
    )
    merged_all[0] = merged.astype(jnp.bfloat16)

    chips = m // 2
    sibling = mine + 1 - 2 * lax.rem(mine, 2)
    piece = length // 2

    def hand(part, source, slot, target):
        rows = pl.ds(part * piece, piece)
        copy = remote(
            merged_all.at[source, rows],
            merged_all.at[slot, rows],
            tp_send_sem.at[part, slot],
            tp_recv_sem.at[part, slot],
            "tp",
            target,
        )
        copy.start()
        return copy

    copies = {}
    for part in range(2):
        for chip in range(1, chips):
            copies[part, chip] = hand(part, 0, chip, lax.rem(mine + 2 * chip, m))
    for part in range(2):
        copies[part, chips] = hand(part, 0, chips, sibling)
    loads[2].wait()

    def term(part, slot):
        chip = slot % chips
        owner = lax.rem((mine if slot < chips else sibling) - 2 * chip + m, m)
        rows = pl.ds(pl.multiple_of(owner * columns, columns), columns)
        return jnp.dot(
            merged_all[slot, part * piece : (part + 1) * piece],
            out_weight[rows, :],
            preferred_element_type=jnp.float32,
        )

    totals = [term(part, 0) for part in range(2)]
    for part in range(2):
        for chip in range(1, chips):
            copies[part, chip].wait()
            copies[part, chips + chip] = hand(part, chip, chips + chip, sibling)
        copies[part, chips].wait()
        totals[part] = totals[part] + term(part, chips)
        for chip in range(1, chips):
            totals[part] = totals[part] + term(part, chip)
    for part in range(2):
        for chip in range(1, chips):
            copies[part, chips + chip].wait()
            totals[part] = totals[part] + term(part, chips + chip)
        result_ref[part * piece : (part + 1) * piece] = totals[part].astype(result_ref.dtype)


def turn_tables(n, length):
    half = HEAD_DIM // 2
    inverse = 1.0 / 10000.0 ** (np.arange(half, dtype=np.float32) * np.float32(2.0) / HEAD_DIM)
    inverse = np.tile(inverse.astype(np.float64), 128 // half)[None]
    inner = np.arange(length)[:, None] * inverse
    outer = (np.arange(n) * length)[:, None] * inverse
    table = np.stack([np.cos(inner), np.sin(inner)]).astype(np.float32)
    base = np.stack([np.cos(outer), np.sin(outer)]).astype(np.float32)
    return table, base


def fused(n, m, tokens, query_weight, key_weight, value_weight, out_weight):
    length, width = tokens.shape
    columns = query_weight.shape[2]
    table, base = turn_tables(n, length)
    steps = length // FAR_DILATION
    classes = FAR_DILATION // n
    kept = columns + 128
    bf16 = jnp.bfloat16
    hbm = pl.BlockSpec(memory_space=pl.ANY)
    vmem = pl.BlockSpec(memory_space=pltpu.VMEM)
    dma = pltpu.SemaphoreType.DMA
    return pl.pallas_call(
        functools.partial(fused_kernel, n, m),
        out_shape=jax.ShapeDtypeStruct((length, out_weight.shape[1]), jnp.float32),
        in_specs=[hbm] * 6 + [vmem],
        out_specs=vmem,
        scratch_shapes=[
            pltpu.VMEM((length, width), bf16),
            pltpu.VMEM((9, width, columns), bf16),
            pltpu.VMEM(out_weight.shape, bf16),
            pltpu.VMEM(table.shape, jnp.float32),
            pltpu.VMEM((2, length + 2 * SIDE_STEPS, columns), bf16),
            pltpu.VMEM((2, MIDDLE_DILATION, 3, length // MIDDLE_DILATION, columns), bf16),
            pltpu.VMEM((3, FAR_DILATION, steps, columns), bf16),
            pltpu.VMEM((3, classes, n, steps, columns), bf16),
            pltpu.VMEM((classes, n, steps, kept), bf16),
            pltpu.VMEM((FAR_DILATION, steps, kept), bf16),
            pltpu.VMEM((m, length, columns), bf16),
            dma((3,)),
            dma((9,)),
            dma((2,)),
            dma((4,)),
            dma((4,)),
            dma((3, n)),
            dma((3, n)),
            dma((n,)),
            dma((n,)),
            dma((2, m)),
            dma((2, m)),
        ],
        compiler_params=pltpu.CompilerParams(
            collective_id=0, has_side_effects=True, vmem_limit_bytes=60 * 1024 * 1024
        ),
    )(tokens, query_weight, key_weight, value_weight, out_weight, jnp.asarray(table), jnp.asarray(base)).astype(bf16)


def planned(n, m, *arrays):
    length, columns = arrays[0].shape[0], arrays[1].shape[2]
    fits = (
        n > 1
        and m % 2 == 0
        and FAR_DILATION % n == 0
        and length == SIDE_STEPS * MIDDLE_DILATION
        and length % (FAR_DILATION * 16) == 0
        and columns % 128 == 0
        and 3 * (columns // HEAD_DIM) <= 128
    )
    if fits:
        return fused(n, m, *arrays)
    return per_device(*arrays)


def solution(mesh):
    placed = (
        P("sp", None),
        P(None, None, "tp"),
        P(None, None, "tp"),
        P(None, None, "tp"),
        P(None, "tp"),
    )
    return jax.shard_map(
        functools.partial(planned, mesh.shape["sp"], mesh.shape["tp"]),
        mesh=mesh,
        in_specs=placed,
        out_specs=P("sp", "tp"),
        check_vma=False,
    )
```
